32 devices in a mesh: dp: 2 (over x), kv: 8 (over z, y), tp: 2 (over core).
Axes of the slice: x: 2, y: 2, z: 4, core: 2. Of those that a mesh axis runs over, the one named last changes fastest.
Arguments:
- tokens: bfloat16 [16, 2048], P('dp', 'kv'), may hold values from -6 to 6
- lengths: int32 [16], P('dp'), may hold values from 1 to 2047, as said below
- query_weight: bfloat16 [2048, 2048], P('kv', 'tp'), may hold values from -0.125 to 0.125
- key_weight: bfloat16 [2048, 256], P('kv', 'tp'), may hold values from -0.125 to 0.125
- value_weight: bfloat16 [2048, 256], P('kv', 'tp'), may hold values from -0.125 to 0.125
- query_gain: float32 [64], replicated, may hold values from 0.1 to 1.9
- key_gain: float32 [64], replicated, may hold values from 0.1 to 1.9
- lambdas: float32 [16], P('tp'), may hold values from 0.3 to 0.8
- head_gain: float32 [128], replicated, may hold values from 0.1 to 1.9
- out_weight: bfloat16 [2048, 2048], P('tp', 'kv'), may hold values from -0.125 to 0.125
- cache_keys: bfloat16 [16, 2048, 2, 128], P('dp', 'kv', 'tp'), may hold values from -400 to 400
- cache_values: bfloat16 [16, 2048, 2, 128], P('dp', 'kv', 'tp'), may hold values from -6 to 6
Outputs:
- mixed: bfloat16 [16, 2048], P('dp', 'kv')
- new_keys: bfloat16 [16, 2, 128], P('dp', 'tp')
- new_values: bfloat16 [16, 2, 128], P('dp', 'tp')
The draws below stay inside these ranges and needn't reach their ends.
Inputs may be any that keep to these rules, and one draw needn't show every extreme that they name: `lengths`: of each index of dp's 8 sequences, the first has 1792 or more cached positions, the second fewer than 16, the others half of 2048 or more.
All inputs are finite; a program needn't handle non-finite values.
Results may differ from the reference program's by a relative error of at most 0.023.
Values may be sent and summed in bfloat16 or wider, within the bound.
A program may use at most 64 MiB of HBM per device.

```python
import math
import jax
import jax.numpy as jnp
from jax import lax

D = 2048
HEADS = 16
KV_HEADS = 2
HEAD = 64
VALUE = 128
SEQ_DEV = 8
POS_DEV = 256
BATCH = 16
CTX = 2048
N_TP = 2


def draw_lengths(key, part):
    slot_index = jnp.arange(BATCH, dtype=jnp.int32) % SEQ_DEV
    longest = jax.random.randint(jax.random.fold_in(key, 11), (BATCH,), CTX - POS_DEV, CTX)
    shortest = jax.random.randint(jax.random.fold_in(key, 12), (BATCH,), 1, 16)
    drawn = jax.random.randint(jax.random.fold_in(key, 13), (BATCH,), CTX // 2, CTX)
    chosen = jnp.where(slot_index == 0, longest, jnp.where(slot_index == 1, shortest, drawn))
    return chosen.astype(jnp.int32)


def draw_cache_keys(key, part):
    shape = (BATCH, CTX, KV_HEADS, VALUE)
    base = jnp.clip(jax.random.normal(jax.random.fold_in(key, 21), shape, jnp.float32) * 1.75, -10.5, 10.5)
    position_ids = jnp.arange(CTX, dtype=jnp.int32)[None, :]
    chosen_place = jax.random.randint(jax.random.fold_in(key, 24), (BATCH, 1), 0, CTX // 2)
    picked = (position_ids == 0) | (position_ids == chosen_place)
    factor = jnp.exp(jax.random.uniform(jax.random.fold_in(key, 23), (BATCH, CTX), jnp.float32, minval=jnp.log(10.0), maxval=jnp.log(35.0)))
    base = jnp.where(picked[:, :, None, None], base * factor[:, :, None, None], base)
    return base.astype(jnp.bfloat16)


def block_levels(key, extent, shards, least, largest):
    level, own = 1.0, jax.random.fold_in(key, 6)
    for dim, parts in shards:
        heights = jnp.exp(jax.random.uniform(jax.random.fold_in(own, dim), (parts,), jnp.float32, least / len(shards), largest / len(shards)))
        level = level * jnp.repeat(heights, extent[dim] // parts).reshape([-1 if axis == dim else 1 for axis in range(len(extent))])
    return level


def bell_draw(stream_key, shape, spread, reach, shards=(), kind=jnp.bfloat16):
    drawn = jax.random.normal(stream_key, shape, jnp.float32) * spread
    if len(shards) > 0:
        drawn = block_levels(stream_key, shape, shards, -0.22, 0.18) * drawn
    return jnp.clip(drawn, min=-reach, max=reach).astype(kind)


def setup_inputs(seed: int = 0) -> dict:
    key_list = jax.random.split(jax.random.key(seed), 13)
    tokens = bell_draw(key_list[0], (BATCH, D), 1.0, 6.0, ((0, 2), (1, 8)))
    lengths = draw_lengths(jax.random.fold_in(key_list[12], 71), 0)
    query_weight = bell_draw(key_list[2], (D, HEADS * VALUE), D ** -0.5, 0.125, ((0, 8), (1, 2)))
    key_weight = bell_draw(key_list[3], (D, KV_HEADS * VALUE), D ** -0.5, 0.125, ((0, 8), (1, 2)))
    value_weight = bell_draw(key_list[4], (D, KV_HEADS * VALUE), D ** -0.5, 0.125, ((0, 8), (1, 2)))
    query_gain = jnp.clip(1.0 + 0.18 * jax.random.normal(key_list[5], (HEAD,), jnp.float32), 0.1, 1.9)
    key_gain = jnp.clip(1.0 + 0.18 * jax.random.normal(key_list[6], (HEAD,), jnp.float32), 0.1, 1.9)
    lambdas = jnp.clip(0.3 + 0.5 * jax.random.uniform(key_list[7], (HEADS,), jnp.float32) ** block_levels(key_list[7], (HEADS,), ((0, 2),), -0.2, 0.2), 0.3, 0.8)
    head_gain = jnp.clip(1.0 + 0.18 * jax.random.normal(key_list[8], (VALUE,), jnp.float32), 0.1, 1.9)
    out_weight = bell_draw(key_list[9], (HEADS * VALUE, D), (HEADS * VALUE) ** -0.5, 0.125, ((0, 2), (1, 8)))
    cache_keys = draw_cache_keys(jax.random.fold_in(key_list[12], 71), 0)
    cache_values = bell_draw(key_list[11], (BATCH, CTX, KV_HEADS, VALUE), 1.0, 6.0, ((0, 2), (1, 8), (2, 2)))
    return {"tokens": tokens, "lengths": lengths, "query_weight": query_weight, "key_weight": key_weight, "value_weight": value_weight, "query_gain": query_gain, "key_gain": key_gain, "lambdas": lambdas, "head_gain": head_gain, "out_weight": out_weight, "cache_keys": cache_keys, "cache_values": cache_values}


epsilon = 1e-06
rotary_base = 10000.0
masked_score = -1e+30
output_scale = 0.2 + 0.6 * math.exp(-0.3)

def new_entries(proj_query, proj_key, proj_value, query_gain, key_gain, lengths):
    rows = proj_query.shape[0]
    head_dim = query_gain.shape[0]
    half_dim = head_dim // 2
    frequency = rotary_base ** (-jnp.arange(half_dim, dtype=jnp.float32) / half_dim)
    angle = lengths.astype(jnp.float32)[:, None, None, None] * frequency
    cosine_term = jnp.cos(angle)
    sine_term = jnp.sin(angle)

    def turned(pieces, gain):
        normed = pieces * lax.rsqrt(lax.optimization_barrier(jnp.mean(pieces * pieces, axis=-1, keepdims=True)) + epsilon) * gain
        lower_part = normed[..., :half_dim]
        upper_part = normed[..., half_dim:]
        return jnp.concatenate([lower_part * cosine_term - upper_part * sine_term, upper_part * cosine_term + lower_part * sine_term], axis=-1)
    queries = turned(proj_query.reshape(rows, -1, 2, head_dim), query_gain).astype(jnp.bfloat16)
    new_keys = turned(proj_key.reshape(rows, -1, 2, head_dim), key_gain).astype(jnp.bfloat16)
    new_values = proj_value.reshape(rows, -1, 2 * head_dim).astype(jnp.bfloat16)
    return (queries, new_keys.reshape(rows, -1, 2 * head_dim), new_values)

def finish_heads(weighted, totals, lambdas, head_gain):
    heads = weighted / totals[..., None]
    gaps = heads[..., 0, :] - lambdas[..., None] * heads[..., 1, :]
    normed = gaps * lax.rsqrt(lax.optimization_barrier(jnp.mean(gaps * gaps, axis=-1, keepdims=True)) + epsilon) * head_gain
    return (normed * output_scale).astype(jnp.bfloat16)

def attend_one(query, keys, values, length, own_key, own_value, lambdas, head_gain):
    positions, kv_heads, width = keys.shape
    head_dim = width // 2
    scale = head_dim ** (-0.5)
    query_wide = query.astype(jnp.float32)
    scores = jnp.einsum('kgtd,pktd->kgtp', query_wide, keys.reshape(positions, kv_heads, 2, head_dim).astype(jnp.float32)) * scale
    valid = jnp.arange(positions, dtype=jnp.int32) < length
    own_score = jnp.einsum('kgtd,ktd->kgt', query_wide, own_key.reshape(kv_heads, 2, head_dim).astype(jnp.float32)) * scale
    highest = jnp.maximum(lax.optimization_barrier(jnp.max(jnp.where(valid, scores, masked_score), axis=-1)), own_score)
    expo = jnp.where(valid, jnp.exp(scores - highest[..., None]), 0.0)
    own_weight = jnp.exp(own_score - highest)
    totals = lax.optimization_barrier(jnp.sum(expo, axis=-1)) + own_weight
    rounded = lax.optimization_barrier(expo.astype(jnp.bfloat16)).astype(jnp.float32)
    weighted = jnp.einsum('kgtp,pke->kgte', rounded, values.astype(jnp.float32))
    weighted = weighted + own_weight[..., None] * own_value.astype(jnp.float32)[:, None, None, :]
    attended = finish_heads(weighted, totals, lambdas.reshape(kv_heads, -1), head_gain)
    return attended.reshape(-1)

def reference(tokens, lengths, query_weight, key_weight, value_weight, query_gain, key_gain, lambdas, head_gain, out_weight, cache_keys, cache_values):
    proj_query = jnp.dot(tokens, query_weight, preferred_element_type=jnp.float32)
    proj_key = jnp.dot(tokens, key_weight, preferred_element_type=jnp.float32)
    proj_value = jnp.dot(tokens, value_weight, preferred_element_type=jnp.float32)
    queries, new_keys, new_values = new_entries(proj_query, proj_key, proj_value, query_gain, key_gain, lengths)
    rows = tokens.shape[0]
    kv_heads = cache_keys.shape[2]
    queries = queries.reshape(rows, kv_heads, -1, 2, queries.shape[-1])
    attended = lax.map(lambda items: attend_one(items[0], items[1], items[2], items[3], items[4], items[5], lambdas, head_gain), (queries, cache_keys, cache_values, lengths, new_keys, new_values))
    group_width = attended.shape[1] // N_TP
    summed = jnp.zeros((rows, out_weight.shape[1]), jnp.float32)
    for group in range(N_TP):
        lo_col = group * group_width
        partial_out = jnp.dot(attended[:, lo_col:lo_col + group_width], out_weight[lo_col:lo_col + group_width], preferred_element_type=jnp.float32).astype(jnp.bfloat16)
        summed = summed + lax.optimization_barrier(partial_out).astype(jnp.float32)
    mixed = summed.astype(jnp.bfloat16)
    return (mixed, new_keys, new_values)
```

```python
import functools
import math

import jax
import jax.numpy as jnp
import numpy as np
from jax import lax
from jax.experimental import pallas as pl
from jax.experimental.pallas import tpu as pltpu
from jax.sharding import PartitionSpec as P

epsilon = 1e-06
rotary_base = 10000.0
masked_score = -1e30
output_scale = 0.2 + 0.6 * math.exp(-0.3)
unroll_limit = 16
f32 = jnp.float32
bf16 = jnp.bfloat16
MESH = pl.DeviceIdType.MESH


def over(lo, hi, step):
    if hi - lo <= unroll_limit:
        for i in range(lo, hi):
            step(i)
    else:

        def one(i, carry):
            step(i)
            return carry

        lax.fori_loop(lo, hi, one, 0)


def gather(n, step, init):
    if n <= unroll_limit:
        for i in range(n):
            init = step(i, init)
        return init
    return lax.fori_loop(0, n, step, init)


def kernel(
    n_kv,
    n_tp,
    lengths,
    lambdas,
    tokens_h,
    wq_h,
    wk_h,
    wv_h,
    freq_h,
    qg_h,
    kg_h,
    hg_h,
    wo_h,
    ck_h,
    cv_h,
    mixed_o,
    nk_o,
    nv_o,
    tokens,
    wq,
    wk,
    wv,
    freq,
    qg,
    kg,
    hg,
    wo,
    ck,
    cv,
    send_a,
    recv_a,
    wide,
    qbuf,
    send_w,
    send_s,
    recv_w,
    recv_s,
    att,
    att_f,
    part,
    load_sem,
    a_send,
    a_recv,
    b_send,
    b_recv,
    w_send,
    w_recv,
    s_send,
    s_recv,
    e_send,
    e_recv,
    t_send,
    t_recv,
):
    me = lax.axis_index("kv")
    core = lax.axis_index("tp")
    rows, positions, width = ck.shape
    half = width // 2
    quarter = half // 2
    heads = wq.shape[1] // width
    slab = heads + 2
    owners = min(n_kv, rows)
    owned = rows // owners
    scale = half ** (-0.5)

    pairs = [
        (tokens_h, tokens),
        (wq_h, wq),
        (wk_h, wk),
        (wv_h, wv),
        (freq_h, freq),
        (qg_h, qg),
        (kg_h, kg),
        (hg_h, hg),
        (ck_h, ck),
        (cv_h, cv),
        (wo_h, wo),
    ]
    loads = [
        pltpu.make_async_copy(src, dst, load_sem.at[i]) for i, (src, dst) in enumerate(pairs)
    ]
    for load in loads:
        load.start()

    barrier = pltpu.get_barrier_semaphore()

    def peer_of(o):
        return lax.rem(me + o, n_kv)

    def greet(o):
        pl.semaphore_signal(barrier, inc=1, device_id={"kv": peer_of(o)}, device_id_type=MESH)

    over(1, n_kv, greet)
    for o in range(1, n_tp):
        pl.semaphore_signal(
            barrier, inc=1, device_id={"tp": lax.rem(core + o, n_tp)}, device_id_type=MESH
        )

    def if_owner(index, run):
        if owners == n_kv:
            run()
        else:
            pl.when(index < owners)(run)

    def remote(src, dst, ssem, rsem, peer):
        return pltpu.make_async_remote_copy(
            src_ref=src,
            dst_ref=dst,
            send_sem=ssem,
            recv_sem=rsem,
            device_id={"kv": peer},
            device_id_type=MESH,
        )

    def rows_of(index):
        return pl.ds(index * owned, owned)

    for load in loads[:4]:
        load.wait()
    x = tokens[...]
    pq = jnp.dot(x, wq[...], preferred_element_type=f32)
    pk = jnp.dot(x, wk[...], preferred_element_type=f32)
    pv = jnp.dot(x, wv[...], preferred_element_type=f32)
    for h in range(heads):
        send_a[:, h, :] = pq[:, h * width : (h + 1) * width]
    send_a[:, heads, :] = pk
    send_a[:, heads + 1, :] = pv

    pl.semaphore_wait(barrier, n_kv - 1 + n_tp - 1)

    def copy_a(peer):
        return remote(
            send_a.at[rows_of(peer)], recv_a.at[me], a_send.at[peer], a_recv.at[me], peer
        )

    def start_a(o):
        peer = peer_of(o)
        if_owner(peer, lambda: copy_a(peer).start())

    over(1, n_kv, start_a)

    lane = lax.broadcasted_iota(jnp.int32, (1, width), 1)
    low_map = lane < half
    low_half = lax.rem(lane, half) < quarter
    eye = lax.broadcasted_iota(jnp.int32, (2 * heads, width), 0) == lax.broadcasted_iota(
        jnp.int32, (2 * heads, width), 1
    )

    def to_lanes(column):
        return jnp.sum(jnp.where(eye, column, 0.0), axis=0, keepdims=True)

    def to_column(line):
        return jnp.sum(jnp.where(eye, line, 0.0), axis=1, keepdims=True)

    for load in loads[4:8]:
        load.wait()

    def own_a():
        gain_q = jnp.concatenate([qg[...], qg[...]], axis=1)
        gain_k = jnp.concatenate([kg[...], kg[...]], axis=1)
        slab_row = lax.broadcasted_iota(jnp.int32, (slab, width), 0)
        gain = jnp.where(slab_row < heads, gain_q, gain_k)
        turns = []
        for j in range(owned):
            angle = lengths[me * owned + j].astype(f32) * freq[...]
            turns.append((jnp.cos(angle), jnp.where(low_half, -1.0, 1.0) * jnp.sin(angle)))
        recv_a[pl.ds(me, 1)] = send_a[rows_of(me)][None]

        def wait_a(o):
            peer = peer_of(o)
            remote(
                send_a.at[rows_of(0)], recv_a.at[peer], a_send.at[0], a_recv.at[peer], peer
            ).wait_recv()

        over(1, n_kv, wait_a)
        wide[...] = jnp.zeros_like(wide)
        for j in range(owned):
            total = gather(n_kv, lambda i, t: t + recv_a[i, j], jnp.zeros((slab, width), f32))
            square = total * total
            mean_lo = jnp.sum(jnp.where(low_map, square, 0.0), axis=1, keepdims=True)
            mean_hi = jnp.sum(jnp.where(low_map, 0.0, square), axis=1, keepdims=True)
            mean = jnp.where(low_map, mean_lo, mean_hi) * (1.0 / half)
            normed = total * lax.rsqrt(mean + epsilon) * gain
            other = jnp.where(
                low_half,
                pltpu.roll(normed, width - quarter, 1),
                pltpu.roll(normed, quarter, 1),
            )
            cosine, sine = turns[j]
            turned = normed * cosine + other * sine
            wide[:slab, :] = jnp.where(slab_row <= heads, turned, total)
            qbuf[pl.ds(me * owned + j, 1)] = wide[...].astype(bf16)[None]

    if_owner(me, own_a)

    def copy_b(peer):
        mine = qbuf.at[rows_of(me)]
        return remote(mine, mine, b_send.at[peer], b_recv.at[me], peer)

    if_owner(me, lambda: over(1, n_kv, lambda o: copy_b(peer_of(o)).start()))

    def arrived(buf, sem):
        def wait(o):
            peer = peer_of(o)

            def run():
                theirs = buf.at[rows_of(peer)]
                remote(theirs, theirs, b_send.at[0], sem.at[peer], peer).wait_recv()

            if_owner(peer, run)

        over(1, n_kv, wait)

    loads[8].wait()
    loads[9].wait()
    arrived(qbuf, b_recv)

    place = me * positions + lax.broadcasted_iota(jnp.int32, (1, positions), 1)
    for s in range(rows):
        q = qbuf[s][:heads].astype(f32)
        both = jnp.concatenate(
            [jnp.where(low_map, q, 0.0), jnp.where(low_map, 0.0, q)], axis=0
        ).astype(bf16)
        scores = (
            lax.dot_general(both, ck[s], (((1,), (1,)), ((), ())), preferred_element_type=f32)
            * scale
        )
        valid = place < lengths[s]
        highest = jnp.max(jnp.where(valid, scores, masked_score), axis=1, keepdims=True)
        expo = jnp.where(valid, jnp.exp(scores - highest), 0.0)
        send_s[s, 0:1, :] = to_lanes(highest)
        send_s[s, 1:2, :] = to_lanes(jnp.sum(expo, axis=1, keepdims=True))
        send_w[s] = jnp.dot(expo.astype(bf16), cv[s], preferred_element_type=f32)

    def copy_w(peer):
        return remote(
            send_w.at[rows_of(peer)], recv_w.at[me], w_send.at[peer], w_recv.at[me], peer
        )

    def copy_s(peer):
        return remote(
            send_s.at[rows_of(peer)], recv_s.at[me], s_send.at[peer], s_recv.at[me], peer
        )

    def start_d(o):
        peer = peer_of(o)

        def run():
            copy_s(peer).start()
            copy_w(peer).start()

        if_owner(peer, run)

    over(1, n_kv, start_d)

    nk_o[...] = jnp.concatenate(
        [qbuf[s].astype(f32)[heads : heads + 1] for s in range(rows)], axis=0
    ).astype(bf16)
    nv_o[...] = jnp.concatenate(
        [qbuf[s].astype(f32)[heads + 1 : heads + 2] for s in range(rows)], axis=0
    ).astype(bf16)

    def own_d():
        recv_w[pl.ds(me, 1)] = send_w[rows_of(me)][None]
        recv_s[pl.ds(me, 1)] = send_s[rows_of(me)][None]
        weigh = jnp.where(lane < heads, 1.0, 0.0)
        for h in range(heads):
            weigh = jnp.where(lane == heads + h, -lambdas[h], weigh)
        owns = []
        for j in range(owned):
            entry = qbuf[pl.ds(me * owned + j, 1)][0].astype(f32)
            dots = entry[:heads] * entry[heads : heads + 1]
            own_lo = jnp.sum(jnp.where(low_map, dots, 0.0), axis=1, keepdims=True)
            own_hi = jnp.sum(jnp.where(low_map, 0.0, dots), axis=1, keepdims=True)
            own = to_lanes(jnp.concatenate([own_lo, own_hi], axis=0) * scale)
            owns.append((own, entry[heads + 1 : heads + 2]))

        def wait_s(o):
            peer = peer_of(o)
            remote(
                send_s.at[rows_of(0)], recv_s.at[peer], s_send.at[0], s_recv.at[peer], peer
            ).wait_recv()

        def wait_w(o):
            peer = peer_of(o)
            remote(
                send_w.at[rows_of(0)], recv_w.at[peer], w_send.at[0], w_recv.at[peer], peer
            ).wait_recv()

        over(1, n_kv, wait_s)
        over(1, n_kv, wait_w)
        for j in range(owned):
            own, new_value = owns[j]
            highest = gather(n_kv, lambda i, m: jnp.maximum(m, recv_s[i, j, 0:1, :]), own)
            own_weight = jnp.exp(own - highest)
            total = gather(
                n_kv,
                lambda i, t: t
                + recv_s[i, j, 1:2, :] * jnp.exp(recv_s[i, j, 0:1, :] - highest),
                own_weight,
            )
            share = weigh / total
            heads_sum = gather(
                n_kv,
                lambda i, t: t
                + recv_w[i, j] * to_column(share * jnp.exp(recv_s[i, j, 0:1, :] - highest)),
                to_column(share * own_weight) * new_value,
            )
            gaps = heads_sum[:heads] + heads_sum[heads:]
            mean = jnp.mean(gaps * gaps, axis=1, keepdims=True)
            normed = gaps * lax.rsqrt(mean + epsilon) * hg[...]
            att[pl.ds(me * owned + j, 1)] = (normed * output_scale).astype(bf16)[None]

    if_owner(me, own_d)

    def copy_e(peer):
        mine = att.at[rows_of(me)]
        return remote(mine, mine, e_send.at[peer], e_recv.at[me], peer)

    if_owner(me, lambda: over(1, n_kv, lambda o: copy_e(peer_of(o)).start()))
    loads[10].wait()
    arrived(att, e_recv)

    att_f[...] = att[...].astype(f32).reshape(rows * heads, width)
    attended = jnp.concatenate(
        [att_f[pl.ds(h, rows, stride=heads), :] for h in range(heads)], axis=1
    ).astype(bf16)
    part[pl.ds(core, 1)] = jnp.dot(attended, wo[...], preferred_element_type=f32).astype(bf16)[
        None
    ]

    def copy_t(peer):
        return pltpu.make_async_remote_copy(
            src_ref=part.at[core],
            dst_ref=part.at[core],
            send_sem=t_send.at[peer],
            recv_sem=t_recv.at[core],
            device_id={"tp": peer},
            device_id_type=MESH,
        )

    for o in range(1, n_tp):
        copy_t(lax.rem(core + o, n_tp)).start()
    for o in range(1, n_tp):
        peer = lax.rem(core + o, n_tp)
        pltpu.make_async_remote_copy(
            src_ref=part.at[peer],
            dst_ref=part.at[peer],
            send_sem=t_send.at[0],
            recv_sem=t_recv.at[peer],
            device_id={"tp": peer},
            device_id_type=MESH,
        ).wait_recv()
    mixed_o[...] = gather(
        n_tp, lambda i, t: t + part[i].astype(f32), jnp.zeros(mixed_o.shape, f32)
    ).astype(bf16)

    def sent(o):
        peer = peer_of(o)

        def run():
            copy_a(peer).wait_send()
            copy_s(peer).wait_send()
            copy_w(peer).wait_send()

        if_owner(peer, run)

    def sent_all(o):
        peer = peer_of(o)
        copy_b(peer).wait_send()
        copy_e(peer).wait_send()

    over(1, n_kv, sent)
    if_owner(me, lambda: over(1, n_kv, sent_all))
    for o in range(1, n_tp):
        copy_t(lax.rem(core + o, n_tp)).wait_send()


def body(
    n_kv,
    n_tp,
    tokens,
    lengths,
    query_weight,
    key_weight,
    value_weight,
    query_gain,
    key_gain,
    lambdas,
    head_gain,
    out_weight,
    cache_keys,
    cache_values,
):
    rows, positions, kv_heads, width = cache_keys.shape
    assert kv_heads == 1 and key_weight.shape[1] == width
    half = width // 2
    quarter = half // 2
    heads = query_weight.shape[1] // width
    owners = min(n_kv, rows)
    assert rows % owners == 0
    owned = rows // owners
    ck = cache_keys.reshape(rows, positions, width)
    cv = cache_values.reshape(rows, positions, width)
    exponent = -(np.arange(width) % quarter) / quarter
    freq = jnp.asarray((rotary_base**exponent).astype(np.float32)[None])
    qg = query_gain.reshape(1, half)
    kg = key_gain.reshape(1, half)
    hg = head_gain.reshape(1, width)
    held = [
        tokens,
        query_weight,
        key_weight,
        value_weight,
        freq,
        qg,
        kg,
        hg,
        out_weight,
        ck,
        cv,
    ]
    dma = pltpu.SemaphoreType.DMA
    smem = pl.BlockSpec(memory_space=pltpu.SMEM)
    hbm = pl.BlockSpec(memory_space=pl.ANY)
    vmem = pl.BlockSpec(memory_space=pltpu.VMEM)
    out_columns = out_weight.shape[1]
    wide_rows = -(-(heads + 2) // 16) * 16
    mixed, new_keys, new_values = pl.pallas_call(
        functools.partial(kernel, n_kv, n_tp),
        name="decode_step",
        out_shape=[
            jax.ShapeDtypeStruct((rows, out_columns), bf16),
            jax.ShapeDtypeStruct((rows, width), bf16),
            jax.ShapeDtypeStruct((rows, width), bf16),
        ],
        in_specs=[smem, smem] + [hbm] * len(held),
        out_specs=[vmem] * 3,
        scratch_shapes=[pltpu.VMEM(a.shape, a.dtype) for a in held]
        + [
            pltpu.VMEM((rows, heads + 2, width), f32),
            pltpu.VMEM((n_kv, owned, heads + 2, width), f32),
            pltpu.VMEM((wide_rows, width), f32),
            pltpu.VMEM((rows, wide_rows, width), bf16),
            pltpu.VMEM((rows, 2 * heads, width), f32),
            pltpu.VMEM((rows, 2, width), f32),
            pltpu.VMEM((n_kv, owned, 2 * heads, width), f32),
            pltpu.VMEM((n_kv, owned, 2, width), f32),
            pltpu.VMEM((rows, heads, width), bf16),
            pltpu.VMEM((rows * heads, width), f32),
            pltpu.VMEM((n_tp, rows, out_columns), bf16),
            dma((len(held),)),
            dma((owners,)),
            dma((n_kv,)),
            dma((n_kv,)),
            dma((owners,)),
            dma((owners,)),
            dma((n_kv,)),
            dma((owners,)),
            dma((n_kv,)),
            dma((n_kv,)),
            dma((owners,)),
            dma((n_tp,)),
            dma((n_tp,)),
        ],
        compiler_params=pltpu.CompilerParams(collective_id=0, has_side_effects=True),
    )(lengths, lambdas, *held)
    return (
        mixed,
        new_keys.reshape(rows, kv_heads, width),
        new_values.reshape(rows, kv_heads, width),
    )


def solution(mesh):
    return jax.shard_map(
        functools.partial(body, mesh.shape["kv"], mesh.shape["tp"]),
        mesh=mesh,
        in_specs=(
            P("dp", "kv"),
            P("dp"),
            P("kv", "tp"),
            P("kv", "tp"),
            P("kv", "tp"),
            P(),
            P(),
            P("tp"),
            P(),
            P("tp", "kv"),
            P("dp", "kv", "tp", None),
            P("dp", "kv", "tp", None),
        ),
        out_specs=(P("dp", "kv"), P("dp", "tp", None), P("dp", "tp", None)),
        check_vma=False,
    )
```

```python
import functools
import math

import jax
import jax.numpy as jnp
import numpy as np
from jax import lax
from jax.experimental import pallas as pl
from jax.experimental.pallas import tpu as pltpu
from jax.sharding import PartitionSpec as P

epsilon = 1e-06
rotary_base = 10000.0
masked_score = -1e30
output_scale = 0.2 + 0.6 * math.exp(-0.3)
unroll_limit = 16
f32 = jnp.float32
bf16 = jnp.bfloat16
MESH = pl.DeviceIdType.MESH


def over(lo, hi, step):
    if hi - lo <= unroll_limit:
        for i in range(lo, hi):
            step(i)
    else:

        def one(i, carry):
            step(i)
            return carry

        lax.fori_loop(lo, hi, one, 0)


def gather(n, step, init):
    if n <= unroll_limit:
        for i in range(n):
            init = step(i, init)
        return init
    return lax.fori_loop(0, n, step, init)


def kernel(
    n_kv,
    n_tp,
    lengths_h,
    lambdas_h,
    tokens_h,
    wq_h,
    wk_h,
    wv_h,
    freq_h,
    qg_h,
    kg_h,
    hg_h,
    ck_h,
    cv_h,
    wo_h,
    mixed_o,
    nk_o,
    nv_o,
    lengths,
    lambdas,
    tokens,
    wq,
    wk,
    wv,
    freq,
    qg,
    kg,
    hg,
    ck,
    cv,
    wo,
    send_a,
    recv_a,
    send_n,
    recv_n,
    qbuf,
    nbuf,
    send_w,
    send_s,
    recv_w,
    recv_s,
    att,
    att_f,
    load_sem,
    a_send,
    a_recv,
    n_send,
    n_recv,
    b_send,
    b_recv,
    k_send,
    k_recv,
    w_send,
    w_recv,
    s_send,
    s_recv,
    e_send,
    e_recv,
    o_send,
    o_recv,
):
    me = lax.axis_index("kv")
    core = lax.axis_index("tp")
    rows, positions, width = ck.shape
    half = width // 2
    quarter = half // 2
    heads = wq.shape[1] // width
    owners, owned, base = owner_plan(n_kv, rows)
    mine = me - base
    is_owner = jnp.logical_and(me >= base, me < base + owners)
    scale = half ** (-0.5)

    pairs = [
        (tokens_h, tokens),
        (wq_h, wq),
        (wk_h, wk),
        (wv_h, wv),
        (lengths_h, lengths),
        (freq_h, freq),
        (qg_h, qg),
        (kg_h, kg),
        (hg_h, hg),
        (lambdas_h, lambdas),
        (ck_h, ck),
        (cv_h, cv),
        (wo_h, wo.at[core]),
    ]
    loads = [
        pltpu.make_async_copy(src, dst, load_sem.at[i]) for i, (src, dst) in enumerate(pairs)
    ]

    barrier = pltpu.get_barrier_semaphore()

    def greet(peer, other):
        pl.semaphore_signal(
            barrier, inc=1, device_id={"kv": peer, "tp": other}, device_id_type=MESH
        )

    def cores():
        return [(lax.rem(core + c, n_tp), c) for c in range(n_tp)]

    def peer_of(o):
        return lax.rem(me + o, n_kv)

    @pl.when(is_owner)
    def _():
        for other, c in cores():
            over(0 if c else 1, n_kv, lambda o: greet(peer_of(o), other))

    @pl.when(jnp.logical_not(is_owner))
    def _():
        for other, c in cores():
            over(0, owners, lambda g: greet(base + g, other))
            if c:
                greet(me, other)

    for load in loads:
        load.start()

    def remote(src, dst, ssem, rsem, peer, other=None):
        return pltpu.make_async_remote_copy(
            src_ref=src,
            dst_ref=dst,
            send_sem=ssem,
            recv_sem=rsem,
            device_id={"kv": peer, "tp": core if other is None else other},
            device_id_type=MESH,
        )

    def rows_of(group):
        return pl.ds(group * owned, owned)

    for load in loads[:4]:
        load.wait()
    x = tokens[...]
    pq = jnp.dot(x, wq[...], preferred_element_type=f32)
    pk = jnp.dot(x, wk[...], preferred_element_type=f32)
    pv = jnp.dot(x, wv[...], preferred_element_type=f32)
    for h in range(heads):
        send_a[:, h, :] = pq[:, h * width : (h + 1) * width]
    send_n[:, 0, :] = pk
    send_n[:, 1, :] = pv

    @pl.when(is_owner)
    def _():
        pl.semaphore_wait(barrier, n_kv * n_tp - 1)

    @pl.when(jnp.logical_not(is_owner))
    def _():
        pl.semaphore_wait(barrier, owners * n_tp + n_tp - 1)

    def copy_a(g):
        return remote(send_a.at[rows_of(g)], recv_a.at[me], a_send.at[g], a_recv.at[me], base + g)

    def copy_n(g):
        return remote(send_n.at[rows_of(g)], recv_n.at[me], n_send.at[g], n_recv.at[me], base + g)

    upper = (2 * me) // n_kv

    def near(t):
        return t + upper * (owners - 1 - 2 * t)

    def start_a(t):
        g = near(owners - 1 - t)

        @pl.when(base + g != me)
        def _():
            copy_a(g).start()
            copy_n(g).start()

    over(0, owners, start_a)

    def copy_o(other):
        return remote(wo_h, wo.at[core], o_send.at[other], o_recv.at[core], me, other)

    for other, c in cores():
        if c:
            copy_o(other).start()

    lane = lax.broadcasted_iota(jnp.int32, (1, width), 1)
    low_map = lane < half
    low_half = lax.rem(lane, half) < quarter
    eye = lax.broadcasted_iota(jnp.int32, (2 * heads, width), 0) == lax.broadcasted_iota(
        jnp.int32, (2 * heads, width), 1
    )

    def to_lanes(column):
        return jnp.sum(jnp.where(eye, column, 0.0), axis=0, keepdims=True)

    def to_column(line):
        return jnp.sum(jnp.where(eye, line, 0.0), axis=1, keepdims=True)

    for load in loads[4:10]:
        load.wait()

    def copy_b(peer):
        ref = qbuf.at[rows_of(mine)]
        return remote(ref, ref, b_send.at[peer], b_recv.at[mine], peer)

    def copy_k(peer):
        ref = nbuf.at[rows_of(mine)]
        return remote(ref, ref, k_send.at[peer], k_recv.at[mine], peer)

    @pl.when(is_owner)
    def _():
        gain_q = jnp.concatenate([qg[...], qg[...]], axis=1)
        gain_k = jnp.concatenate([kg[...], kg[...]], axis=1)
        turns = []
        for j in range(owned):
            angle = lengths[mine * owned + j].astype(f32) * freq[...]
            turns.append((jnp.cos(angle), jnp.where(low_half, -1.0, 1.0) * jnp.sin(angle)))
        recv_a[pl.ds(me, 1)] = send_a[rows_of(mine)][None]
        recv_n[pl.ds(me, 1)] = send_n[rows_of(mine)][None]

        def turned(total, gain, turn):
            square = total * total
            mean_lo = jnp.sum(jnp.where(low_map, square, 0.0), axis=1, keepdims=True)
            mean_hi = jnp.sum(jnp.where(low_map, 0.0, square), axis=1, keepdims=True)
            mean = jnp.where(low_map, mean_lo, mean_hi) * (1.0 / half)
            normed = total * lax.rsqrt(mean + epsilon) * gain
            other = jnp.where(
                low_half,
                pltpu.roll(normed, width - quarter, 1),
                pltpu.roll(normed, quarter, 1),
            )
            return normed * turn[0] + other * turn[1]

        def wait_a(o):
            peer = peer_of(o)
            remote(
                send_a.at[rows_of(0)], recv_a.at[peer], a_send.at[0], a_recv.at[peer], peer
            ).wait_recv()

        def wait_n(o):
            peer = peer_of(o)
            remote(
                send_n.at[rows_of(0)], recv_n.at[peer], n_send.at[0], n_recv.at[peer], peer
            ).wait_recv()

        over(1, n_kv, wait_a)
        for j in range(owned):
            total = gather(n_kv, lambda i, t: t + recv_a[i, j], jnp.zeros((heads, width), f32))
            qbuf[pl.ds(mine * owned + j, 1)] = turned(total, gain_q, turns[j]).astype(bf16)[None]
        over(1, n_kv, lambda o: copy_b(peer_of(o)).start())
        over(1, n_kv, wait_n)
        first = lax.broadcasted_iota(jnp.int32, (2, width), 0) == 0
        for j in range(owned):
            total = gather(n_kv, lambda i, t: t + recv_n[i, j], jnp.zeros((2, width), f32))
            entry = jnp.where(first, turned(total, gain_k, turns[j]), total)
            nbuf[pl.ds(mine * owned + j, 1)] = entry.astype(bf16)[None]
        over(1, n_kv, lambda o: copy_k(peer_of(o)).start())

    def arrive(buf, sem, g):
        ref = buf.at[rows_of(g)]
        remote(ref, ref, b_send.at[0], sem.at[g], base + g).wait_recv()

    loads[10].wait()
    loads[11].wait()

    def copy_w(g):
        return remote(send_w.at[rows_of(g)], recv_w.at[me], w_send.at[g], w_recv.at[me], base + g)

    def copy_s(g):
        return remote(send_s.at[rows_of(g)], recv_s.at[me], s_send.at[g], s_recv.at[me], base + g)

    place = me * positions + lax.broadcasted_iota(jnp.int32, (1, positions), 1)

    def attend(t):
        g = near(t)

        @pl.when(base + g != me)
        def _():
            arrive(qbuf, b_recv, g)

        for j in range(owned):
            s = g * owned + j
            q = qbuf[pl.ds(s, 1)][0].astype(f32)
            both = jnp.concatenate(
                [jnp.where(low_map, q, 0.0), jnp.where(low_map, 0.0, q)], axis=0
            ).astype(bf16)
            scores = (
                lax.dot_general(
                    both,
                    ck[pl.ds(s, 1)][0],
                    (((1,), (1,)), ((), ())),
                    preferred_element_type=f32,
                )
                * scale
            )
            valid = place < lengths[s]
            highest = jnp.max(jnp.where(valid, scores, masked_score), axis=1, keepdims=True)
            expo = jnp.where(valid, jnp.exp(scores - highest), 0.0)
            summed = jnp.sum(expo, axis=1, keepdims=True)
            send_s[pl.ds(s, 1)] = jnp.concatenate([to_lanes(highest), to_lanes(summed)], axis=0)[
                None
            ]
            send_w[pl.ds(s, 1)] = jnp.dot(
                expo.astype(bf16), cv[pl.ds(s, 1)][0], preferred_element_type=f32
            ).astype(bf16)[None]

        @pl.when(base + g != me)
        def _():
            copy_s(g).start()
            copy_w(g).start()

    over(0, owners, attend)

    def arrive_k(g):
        @pl.when(base + g != me)
        def _():
            arrive(nbuf, k_recv, g)

    over(0, owners, arrive_k)
    entries = [nbuf[s].astype(f32) for s in range(rows)]
    nk_o[...] = jnp.concatenate([e[0:1] for e in entries], axis=0).astype(bf16)
    nv_o[...] = jnp.concatenate([e[1:2] for e in entries], axis=0).astype(bf16)

    def copy_e(peer, other):
        ref = att.at[core, rows_of(mine)]
        return remote(
            ref,
            ref,
            e_send.at[peer * n_tp + other],
            e_recv.at[mine * n_tp + core],
            peer,
            other,
        )

    def each_e(run):
        for other, c in cores():
            over(0 if c else 1, n_kv, lambda o: run(copy_e(peer_of(o), other)))

    @pl.when(is_owner)
    def _():
        recv_w[pl.ds(me, 1)] = send_w[rows_of(mine)][None]
        recv_s[pl.ds(me, 1)] = send_s[rows_of(mine)][None]
        weigh = jnp.where(lane < heads, 1.0, 0.0)
        for h in range(heads):
            weigh = jnp.where(lane == heads + h, -lambdas[h], weigh)
        owns = []
        for j in range(owned):
            query = qbuf[pl.ds(mine * owned + j, 1)][0].astype(f32)
            entry = nbuf[pl.ds(mine * owned + j, 1)][0].astype(f32)
            dots = query * entry[0:1]
            own_lo = jnp.sum(jnp.where(low_map, dots, 0.0), axis=1, keepdims=True)
            own_hi = jnp.sum(jnp.where(low_map, 0.0, dots), axis=1, keepdims=True)
            own = to_lanes(jnp.concatenate([own_lo, own_hi], axis=0) * scale)
            owns.append((own, entry[1:2]))

        def wait_s(o):
            peer = peer_of(o)
            remote(
                send_s.at[rows_of(0)], recv_s.at[peer], s_send.at[0], s_recv.at[peer], peer
            ).wait_recv()

        def wait_w(o):
            peer = peer_of(o)
            remote(
                send_w.at[rows_of(0)], recv_w.at[peer], w_send.at[0], w_recv.at[peer], peer
            ).wait_recv()

        over(1, n_kv, wait_s)
        shares = []
        for j in range(owned):
            own, new_value = owns[j]
            highest = gather(n_kv, lambda i, m: jnp.maximum(m, recv_s[i, j, 0:1, :]), own)
            own_weight = jnp.exp(own - highest)
            total = gather(
                n_kv,
                lambda i, t: t
                + recv_s[i, j, 1:2, :] * jnp.exp(recv_s[i, j, 0:1, :] - highest),
                own_weight,
            )
            share = weigh / total
            shares.append((highest, share, to_column(share * own_weight) * new_value))
        over(1, n_kv, wait_w)
        for j in range(owned):
            highest, share, start = shares[j]
            both = gather(
                n_kv,
                lambda i, t: t
                + recv_w[i, j].astype(f32)
                * to_column(share * jnp.exp(recv_s[i, j, 0:1, :] - highest)),
                start,
            )
            gaps = both[:heads] + both[heads:]
            mean = jnp.mean(gaps * gaps, axis=1, keepdims=True)
            normed = gaps * lax.rsqrt(mean + epsilon) * hg[...]
            att[core, pl.ds(mine * owned + j, 1)] = (normed * output_scale).astype(bf16)[None]
        each_e(lambda copy: copy.start())

    loads[12].wait()

    def project(other, c):
        def wait(g):
            def run():
                ref = att.at[other, rows_of(g)]
                remote(
                    ref, ref, e_send.at[0], e_recv.at[g * n_tp + other], base + g, other
                ).wait_recv()

            if c:
                run()
            else:
                pl.when(base + g != me)(run)

        over(0, owners, wait)
        att_f[...] = att[pl.ds(other, 1)][0].astype(f32).reshape(rows * heads, width)
        attended = jnp.concatenate(
            [att_f[pl.ds(h, rows, stride=heads), :] for h in range(heads)], axis=1
        ).astype(bf16)
        part = jnp.dot(attended, wo[pl.ds(other, 1)][0], preferred_element_type=f32)
        return part.astype(bf16).astype(f32)

    for other, c in cores():
        if c:
            remote(
                wo_h, wo.at[other], o_send.at[0], o_recv.at[other], me, other
            ).wait_recv()
    mixed = jnp.zeros(mixed_o.shape, f32)
    for other, c in cores():
        mixed = mixed + project(other, c)
    mixed_o[...] = mixed.astype(bf16)

    def sent(g):
        @pl.when(base + g != me)
        def _():
            copy_a(g).wait_send()
            copy_n(g).wait_send()
            copy_s(g).wait_send()
            copy_w(g).wait_send()

    over(0, owners, sent)

    @pl.when(is_owner)
    def _():
        def sent_all(o):
            copy_b(peer_of(o)).wait_send()
            copy_k(peer_of(o)).wait_send()

        over(1, n_kv, sent_all)
        each_e(lambda copy: copy.wait_send())

    for other, c in cores():
        if c:
            copy_o(other).wait_send()


def owner_plan(n_kv, rows):
    owners = max(1, min(n_kv // 2, rows))
    return owners, rows // owners, (n_kv - owners) // 2


def emit(*refs):
    count = (len(refs) - 1) // 2
    sem = refs[-1]
    copies = [
        pltpu.make_async_copy(refs[i], refs[count + i], sem.at[i]) for i in range(count)
    ]
    for copy in copies:
        copy.start()
    for copy in copies:
        copy.wait()


def body(
    n_kv,
    n_tp,
    tokens,
    lengths,
    query_weight,
    key_weight,
    value_weight,
    query_gain,
    key_gain,
    lambdas,
    head_gain,
    out_weight,
    cache_keys,
    cache_values,
):
    rows, positions, kv_heads, width = cache_keys.shape
    assert kv_heads == 1 and key_weight.shape[1] == width
    half = width // 2
    quarter = half // 2
    heads = query_weight.shape[1] // width
    owners, owned, _ = owner_plan(n_kv, rows)
    assert owners * owned == rows
    ck = cache_keys.reshape(rows, positions, width)
    cv = cache_values.reshape(rows, positions, width)
    exponent = -(np.arange(width) % quarter) / quarter
    freq = jnp.asarray((rotary_base**exponent).astype(np.float32)[None])
    qg = query_gain.reshape(1, half)
    kg = key_gain.reshape(1, half)
    hg = head_gain.reshape(1, width)
    held = [tokens, query_weight, key_weight, value_weight, freq, qg, kg, hg, ck, cv]
    dma = pltpu.SemaphoreType.DMA
    hbm = pl.BlockSpec(memory_space=pl.ANY)
    vmem = pl.BlockSpec(memory_space=pltpu.VMEM)
    out_columns = out_weight.shape[1]
    shapes = [(rows, out_columns), (rows, width), (rows, width)]
    results = pl.pallas_call(
        functools.partial(kernel, n_kv, n_tp),
        name="decode_step",
        out_shape=[pltpu.VMEM(shape, bf16) for shape in shapes],
        in_specs=[hbm] * (3 + len(held)),
        out_specs=[vmem] * 3,
        scratch_shapes=[
            pltpu.SMEM(lengths.shape, lengths.dtype),
            pltpu.SMEM(lambdas.shape, lambdas.dtype),
        ]
        + [pltpu.VMEM(a.shape, a.dtype) for a in held]
        + [
            pltpu.VMEM((n_tp, *out_weight.shape), bf16),
            pltpu.VMEM((rows, heads, width), f32),
            pltpu.VMEM((n_kv, owned, heads, width), f32),
            pltpu.VMEM((rows, 2, width), f32),
            pltpu.VMEM((n_kv, owned, 2, width), f32),
            pltpu.VMEM((rows, heads, width), bf16),
            pltpu.VMEM((rows, 2, width), bf16),
            pltpu.VMEM((rows, 2 * heads, width), bf16),
            pltpu.VMEM((rows, 2, width), f32),
            pltpu.VMEM((n_kv, owned, 2 * heads, width), bf16),
            pltpu.VMEM((n_kv, owned, 2, width), f32),
            pltpu.VMEM((n_tp, rows, heads, width), bf16),
            pltpu.VMEM((rows * heads, width), f32),
            dma((3 + len(held),)),
            dma((owners,)),
            dma((n_kv,)),
            dma((owners,)),
            dma((n_kv,)),
            dma((n_kv,)),
            dma((owners,)),
            dma((n_kv,)),
            dma((owners,)),
            dma((owners,)),
            dma((n_kv,)),
            dma((owners,)),
            dma((n_kv,)),
            dma((n_kv * n_tp,)),
            dma((owners * n_tp,)),
            dma((n_tp,)),
            dma((n_tp,)),
        ],
        compiler_params=pltpu.CompilerParams(collective_id=0, has_side_effects=True),
    )(lengths, lambdas, *held, out_weight)
    mixed, new_keys, new_values = pl.pallas_call(
        emit,
        name="emit",
        out_shape=[jax.ShapeDtypeStruct(shape, bf16) for shape in shapes],
        in_specs=[vmem] * 3,
        out_specs=[hbm] * 3,
        scratch_shapes=[dma((3,))],
    )(*[pltpu.with_memory_space_constraint(r, pltpu.VMEM) for r in results])
    return (
        mixed,
        new_keys.reshape(rows, kv_heads, width),
        new_values.reshape(rows, kv_heads, width),
    )


def solution(mesh):
    return jax.shard_map(
        functools.partial(body, mesh.shape["kv"], mesh.shape["tp"]),
        mesh=mesh,
        in_specs=(
            P("dp", "kv"),
            P("dp"),
            P("kv", "tp"),
            P("kv", "tp"),
            P("kv", "tp"),
            P(),
            P(),
            P("tp"),
            P(),
            P("tp", "kv"),
            P("dp", "kv", "tp", None),
            P("dp", "kv", "tp", None),
        ),
        out_specs=(P("dp", "kv"), P("dp", "tp", None), P("dp", "tp", None)),
        check_vma=False,
    )
```

```python
import functools
import math

import jax
import jax.numpy as jnp
import numpy as np
from jax import lax
from jax.experimental import pallas as pl
from jax.experimental.pallas import tpu as pltpu
from jax.sharding import PartitionSpec as P

epsilon = 1e-06
rotary_base = 10000.0
masked_score = -1e30
output_scale = 0.2 + 0.6 * math.exp(-0.3)
unroll_limit = 16
f32 = jnp.float32
bf16 = jnp.bfloat16
MESH = pl.DeviceIdType.MESH


def over(lo, hi, step):
    if hi - lo <= unroll_limit:
        for i in range(lo, hi):
            step(i)
    else:

        def one(i, carry):
            step(i)
            return carry

        lax.fori_loop(lo, hi, one, 0)


def gather(n, step, init):
    if n <= unroll_limit:
        for i in range(n):
            init = step(i, init)
        return init
    return lax.fori_loop(0, n, step, init)


def kernel(
    n_kv,
    n_tp,
    lengths_h,
    lambdas_h,
    tokens_h,
    wq_h,
    wk_h,
    wv_h,
    freq_h,
    qg_h,
    kg_h,
    hg_h,
    ck_h,
    cv_h,
    wo_h,
    mixed_o,
    nk_o,
    nv_o,
    lengths,
    lambdas,
    tokens,
    wq,
    wk,
    wv,
    freq,
    qg,
    kg,
    hg,
    ck,
    cv,
    wo,
    send_a,
    recv_a,
    send_n,
    recv_n,
    qbuf,
    nbuf,
    send_w,
    send_s,
    recv_w,
    recv_s,
    att,
    att_f,
    keys_t,
    bias,
    load_sem,
    a_send,
    a_recv,
    n_send,
    n_recv,
    b_send,
    b_recv,
    k_send,
    k_recv,
    w_send,
    w_recv,
    s_send,
    s_recv,
    e_send,
    e_recv,
    o_send,
    o_recv,
):
    me = lax.axis_index("kv")
    core = lax.axis_index("tp")
    rows, positions, width = ck.shape
    half = width // 2
    quarter = half // 2
    heads = wq.shape[1] // width
    owners, owned, base = owner_plan(n_kv, rows)
    mine = me - base
    is_owner = jnp.logical_and(me >= base, me < base + owners)
    scale = half ** (-0.5)

    pairs = [
        (tokens_h, tokens),
        (wq_h, wq),
        (wk_h, wk),
        (wv_h, wv),
        (lengths_h, lengths),
        (freq_h, freq),
        (qg_h, qg),
        (kg_h, kg),
        (hg_h, hg),
        (lambdas_h, lambdas),
        (ck_h, ck),
        (cv_h, cv),
        (wo_h, wo.at[core]),
    ]
    loads = [
        pltpu.make_async_copy(src, dst, load_sem.at[i]) for i, (src, dst) in enumerate(pairs)
    ]

    barrier = pltpu.get_barrier_semaphore()

    def greet(peer, other):
        pl.semaphore_signal(
            barrier, inc=1, device_id={"kv": peer, "tp": other}, device_id_type=MESH
        )

    def cores():
        return [(lax.rem(core + c, n_tp), c) for c in range(n_tp)]

    def peer_of(o):
        return lax.rem(me + o, n_kv)

    def far(o):
        swing = (o // 2) * (2 * (o % 2) - 1)
        return lax.rem(me + n_kv // 2 + swing + n_kv, n_kv)

    @pl.when(is_owner)
    def _():
        for other, c in cores():
            over(0 if c else 1, n_kv, lambda o: greet(peer_of(o), other))

    @pl.when(jnp.logical_not(is_owner))
    def _():
        for other, c in cores():
            over(0, owners, lambda g: greet(base + g, other))
            if c:
                greet(me, other)

    for load in loads:
        load.start()

    def remote(src, dst, ssem, rsem, peer, other=None):
        return pltpu.make_async_remote_copy(
            src_ref=src,
            dst_ref=dst,
            send_sem=ssem,
            recv_sem=rsem,
            device_id={"kv": peer, "tp": core if other is None else other},
            device_id_type=MESH,
        )

    def rows_of(group):
        return pl.ds(group * owned, owned)

    for load in loads[:4]:
        load.wait()
    x = tokens[...]
    pq = jnp.dot(x, wq[...], preferred_element_type=f32)
    pk = jnp.dot(x, wk[...], preferred_element_type=f32)
    pv = jnp.dot(x, wv[...], preferred_element_type=f32)
    for h in range(heads):
        send_a[:, h, :] = pq[:, h * width : (h + 1) * width]
    send_n[:, 0, :] = pk
    send_n[:, 1, :] = pv

    @pl.when(is_owner)
    def _():
        pl.semaphore_wait(barrier, n_kv * n_tp - 1)

    @pl.when(jnp.logical_not(is_owner))
    def _():
        pl.semaphore_wait(barrier, owners * n_tp + n_tp - 1)

    def copy_a(g):
        return remote(send_a.at[rows_of(g)], recv_a.at[me], a_send.at[g], a_recv.at[me], base + g)

    def copy_n(g):
        return remote(send_n.at[rows_of(g)], recv_n.at[me], n_send.at[g], n_recv.at[me], base + g)

    upper = (2 * me) // n_kv

    swap = (me + upper) % 2 if owners % 2 == 0 else 0

    def near(t):
        t = t + swap * (1 - 2 * (t % 2))
        return t + upper * (owners - 1 - 2 * t)

    def start_a(t):
        g = near(owners - 1 - t)

        @pl.when(base + g != me)
        def _():
            copy_a(g).start()

    def start_n(t):
        g = near(owners - 1 - t)

        @pl.when(base + g != me)
        def _():
            copy_n(g).start()

    over(0, owners, start_a)
    over(0, owners, start_n)

    def copy_o(other):
        return remote(wo_h, wo.at[core], o_send.at[other], o_recv.at[core], me, other)

    for other, c in cores():
        if c:
            copy_o(other).start()

    lane = lax.broadcasted_iota(jnp.int32, (1, width), 1)
    low_map = lane < half
    low_half = lax.rem(lane, half) < quarter
    eye = lax.broadcasted_iota(jnp.int32, (2 * heads, width), 0) == lax.broadcasted_iota(
        jnp.int32, (2 * heads, width), 1
    )

    def to_lanes(column):
        return jnp.sum(jnp.where(eye, column, 0.0), axis=0, keepdims=True)

    def to_column(line):
        return jnp.sum(jnp.where(eye, line, 0.0), axis=1, keepdims=True)

    for load in loads[4:10]:
        load.wait()

    loads[10].wait()
    for s in range(rows):
        keys_t[s] = ck[s].T
    place = me * positions + lax.broadcasted_iota(jnp.int32, (1, positions), 1)
    for s in range(rows):
        bias[s] = jnp.where(place < lengths[s], 0.0, masked_score)

    def copy_b(peer):
        ref = qbuf.at[rows_of(mine)]
        return remote(ref, ref, b_send.at[peer], b_recv.at[mine], peer)

    def copy_k(peer):
        ref = nbuf.at[rows_of(mine)]
        return remote(ref, ref, k_send.at[peer], k_recv.at[mine], peer)

    @pl.when(is_owner)
    def _():
        gain_q = jnp.concatenate([qg[...], qg[...]], axis=1)
        gain_k = jnp.concatenate([kg[...], kg[...]], axis=1)
        turns = []
        for j in range(owned):
            angle = lengths[mine * owned + j].astype(f32) * freq[...]
            turns.append((jnp.cos(angle), jnp.where(low_half, -1.0, 1.0) * jnp.sin(angle)))
        recv_a[pl.ds(me, 1)] = send_a[rows_of(mine)][None]
        recv_n[pl.ds(me, 1)] = send_n[rows_of(mine)][None]

        def turned(total, gain, turn):
            square = total * total
            mean_lo = jnp.sum(jnp.where(low_map, square, 0.0), axis=1, keepdims=True)
            mean_hi = jnp.sum(jnp.where(low_map, 0.0, square), axis=1, keepdims=True)
            mean = jnp.where(low_map, mean_lo, mean_hi) * (1.0 / half)
            normed = total * lax.rsqrt(mean + epsilon) * gain
            other = jnp.where(
                low_half,
                pltpu.roll(normed, width - quarter, 1),
                pltpu.roll(normed, quarter, 1),
            )
            return normed * turn[0] + other * turn[1]

        def wait_a(o):
            peer = peer_of(o)
            remote(
                send_a.at[rows_of(0)], recv_a.at[peer], a_send.at[0], a_recv.at[peer], peer
            ).wait_recv()

        def wait_n(o):
            peer = peer_of(o)
            remote(
                send_n.at[rows_of(0)], recv_n.at[peer], n_send.at[0], n_recv.at[peer], peer
            ).wait_recv()

        over(1, n_kv, wait_a)
        for j in range(owned):
            total = gather(n_kv, lambda i, t: t + recv_a[i, j], jnp.zeros((heads, width), f32))
            qbuf[pl.ds(mine * owned + j, 1)] = turned(total, gain_q, turns[j]).astype(bf16)[None]
        over(1, n_kv, lambda o: copy_b(far(o)).start())
        over(1, n_kv, wait_n)
        first = lax.broadcasted_iota(jnp.int32, (2, width), 0) == 0
        for j in range(owned):
            total = gather(n_kv, lambda i, t: t + recv_n[i, j], jnp.zeros((2, width), f32))
            entry = jnp.where(first, turned(total, gain_k, turns[j]), total)
            nbuf[pl.ds(mine * owned + j, 1)] = entry.astype(bf16)[None]
        over(1, n_kv, lambda o: copy_k(far(o)).start())

    def arrive(buf, sem, g):
        ref = buf.at[rows_of(g)]
        remote(ref, ref, b_send.at[0], sem.at[g], base + g).wait_recv()

    loads[11].wait()

    def copy_w(g):
        return remote(send_w.at[rows_of(g)], recv_w.at[me], w_send.at[g], w_recv.at[me], base + g)

    def copy_s(g):
        return remote(send_s.at[rows_of(g)], recv_s.at[me], s_send.at[g], s_recv.at[me], base + g)

    def attend(t):
        g = near(t)

        @pl.when(base + g != me)
        def _():
            arrive(qbuf, b_recv, g)

        for j in range(owned):
            s = g * owned + j
            q = qbuf[pl.ds(s, 1)][0].astype(f32)
            both = jnp.concatenate(
                [jnp.where(low_map, q, 0.0), jnp.where(low_map, 0.0, q)], axis=0
            ).astype(bf16)
            dots = jnp.dot(both, keys_t[pl.ds(s, 1)][0], preferred_element_type=f32)
            scores = dots * scale + bias[pl.ds(s, 1)][0]
            highest = jnp.max(scores, axis=1, keepdims=True)
            expo = jnp.exp(scores - highest)
            summed = jnp.sum(expo, axis=1, keepdims=True)
            send_s[pl.ds(s, 1)] = jnp.concatenate([to_lanes(highest), to_lanes(summed)], axis=0)[
                None
            ]
            send_w[pl.ds(s, 1)] = jnp.dot(
                expo.astype(bf16), cv[pl.ds(s, 1)][0], preferred_element_type=f32
            ).astype(bf16)[None]

        @pl.when(base + g != me)
        def _():
            copy_s(g).start()
            copy_w(g).start()

    over(0, owners, attend)

    def arrive_k(g):
        @pl.when(base + g != me)
        def _():
            arrive(nbuf, k_recv, g)

    over(0, owners, arrive_k)
    entries = [nbuf[s].astype(f32) for s in range(rows)]
    nk_o[...] = jnp.concatenate([e[0:1] for e in entries], axis=0).astype(bf16)
    nv_o[...] = jnp.concatenate([e[1:2] for e in entries], axis=0).astype(bf16)

    def copy_e(peer, other):
        ref = att.at[core, rows_of(mine)]
        return remote(
            ref,
            ref,
            e_send.at[peer * n_tp + other],
            e_recv.at[mine * n_tp + core],
            peer,
            other,
        )

    def each_e(run):
        def each(o):
            for other, _ in cores():
                run(copy_e(far(o), other))

        over(1, n_kv, each)
        for other, c in cores():
            if c:
                run(copy_e(me, other))

    @pl.when(is_owner)
    def _():
        recv_w[pl.ds(me, 1)] = send_w[rows_of(mine)][None]
        recv_s[pl.ds(me, 1)] = send_s[rows_of(mine)][None]
        weigh = jnp.where(lane < heads, 1.0, 0.0)
        for h in range(heads):
            weigh = jnp.where(lane == heads + h, -lambdas[h], weigh)
        owns = []
        for j in range(owned):
            query = qbuf[pl.ds(mine * owned + j, 1)][0].astype(f32)
            entry = nbuf[pl.ds(mine * owned + j, 1)][0].astype(f32)
            dots = query * entry[0:1]
            own_lo = jnp.sum(jnp.where(low_map, dots, 0.0), axis=1, keepdims=True)
            own_hi = jnp.sum(jnp.where(low_map, 0.0, dots), axis=1, keepdims=True)
            own = to_lanes(jnp.concatenate([own_lo, own_hi], axis=0) * scale)
            owns.append((own, entry[1:2]))

        def wait_s(o):
            peer = peer_of(o)
            remote(
                send_s.at[rows_of(0)], recv_s.at[peer], s_send.at[0], s_recv.at[peer], peer
            ).wait_recv()

        def wait_w(o):
            peer = peer_of(o)
            remote(
                send_w.at[rows_of(0)], recv_w.at[peer], w_send.at[0], w_recv.at[peer], peer
            ).wait_recv()

        over(1, n_kv, wait_s)
        shares = []
        for j in range(owned):
            own, new_value = owns[j]
            highest = gather(n_kv, lambda i, m: jnp.maximum(m, recv_s[i, j, 0:1, :]), own)
            own_weight = jnp.exp(own - highest)
            total = gather(
                n_kv,
                lambda i, t: t
                + recv_s[i, j, 1:2, :] * jnp.exp(recv_s[i, j, 0:1, :] - highest),
                own_weight,
            )
            share = weigh / total
            shares.append((highest, share, to_column(share * own_weight) * new_value))
        over(1, n_kv, wait_w)
        for j in range(owned):
            highest, share, start = shares[j]
            both = gather(
                n_kv,
                lambda i, t: t
                + recv_w[i, j].astype(f32)
                * to_column(share * jnp.exp(recv_s[i, j, 0:1, :] - highest)),
                start,
            )
            gaps = both[:heads] + both[heads:]
            mean = jnp.mean(gaps * gaps, axis=1, keepdims=True)
            normed = gaps * lax.rsqrt(mean + epsilon) * hg[...]
            att[core, pl.ds(mine * owned + j, 1)] = (normed * output_scale).astype(bf16)[None]
        each_e(lambda copy: copy.start())

    loads[12].wait()

    def project(other, c):
        def wait(g):
            def run():
                ref = att.at[other, rows_of(g)]
                remote(
                    ref, ref, e_send.at[0], e_recv.at[g * n_tp + other], base + g, other
                ).wait_recv()

            if c:
                run()
            else:
                pl.when(base + g != me)(run)

        over(0, owners, wait)
        att_f[...] = att[pl.ds(other, 1)][0].astype(f32).reshape(rows * heads, width)
        attended = jnp.concatenate(
            [att_f[pl.ds(h, rows, stride=heads), :] for h in range(heads)], axis=1
        ).astype(bf16)
        part = jnp.dot(attended, wo[pl.ds(other, 1)][0], preferred_element_type=f32)
        return part.astype(bf16).astype(f32)

    for other, c in cores():
        if c:
            remote(
                wo_h, wo.at[other], o_send.at[0], o_recv.at[other], me, other
            ).wait_recv()
    mixed = jnp.zeros(mixed_o.shape, f32)
    for other, c in cores():
        mixed = mixed + project(other, c)
    mixed_o[...] = mixed.astype(bf16)

    def sent(g):
        @pl.when(base + g != me)
        def _():
            copy_a(g).wait_send()
            copy_n(g).wait_send()
            copy_s(g).wait_send()
            copy_w(g).wait_send()

    over(0, owners, sent)

    @pl.when(is_owner)
    def _():
        def sent_all(o):
            copy_b(peer_of(o)).wait_send()
            copy_k(peer_of(o)).wait_send()

        over(1, n_kv, sent_all)
        each_e(lambda copy: copy.wait_send())

    for other, c in cores():
        if c:
            copy_o(other).wait_send()


def owner_plan(n_kv, rows):
    owners = max(1, min(n_kv // 2, rows))
    return owners, rows // owners, (n_kv - owners) // 2


def emit(*refs):
    count = (len(refs) - 1) // 2
    sem = refs[-1]
    copies = [
        pltpu.make_async_copy(refs[i], refs[count + i], sem.at[i]) for i in range(count)
    ]
    for copy in copies:
        copy.start()
    for copy in copies:
        copy.wait()


def body(
    n_kv,
    n_tp,
    tokens,
    lengths,
    query_weight,
    key_weight,
    value_weight,
    query_gain,
    key_gain,
    lambdas,
    head_gain,
    out_weight,
    cache_keys,
    cache_values,
):
    rows, positions, kv_heads, width = cache_keys.shape
    assert kv_heads == 1 and key_weight.shape[1] == width
    half = width // 2
    quarter = half // 2
    heads = query_weight.shape[1] // width
    owners, owned, _ = owner_plan(n_kv, rows)
    assert owners * owned == rows
    ck = cache_keys.reshape(rows, positions, width)
    cv = cache_values.reshape(rows, positions, width)
    exponent = -(np.arange(width) % quarter) / quarter
    freq = jnp.asarray((rotary_base**exponent).astype(np.float32)[None])
    qg = query_gain.reshape(1, half)
    kg = key_gain.reshape(1, half)
    hg = head_gain.reshape(1, width)
    held = [tokens, query_weight, key_weight, value_weight, freq, qg, kg, hg, ck, cv]
    dma = pltpu.SemaphoreType.DMA
    hbm = pl.BlockSpec(memory_space=pl.ANY)
    vmem = pl.BlockSpec(memory_space=pltpu.VMEM)
    out_columns = out_weight.shape[1]
    shapes = [(rows, out_columns), (rows, width), (rows, width)]
    results = pl.pallas_call(
        functools.partial(kernel, n_kv, n_tp),
        name="decode_step",
        out_shape=[pltpu.VMEM(shape, bf16) for shape in shapes],
        in_specs=[hbm] * (3 + len(held)),
        out_specs=[vmem] * 3,
        scratch_shapes=[
            pltpu.SMEM(lengths.shape, lengths.dtype),
            pltpu.SMEM(lambdas.shape, lambdas.dtype),
        ]
        + [pltpu.VMEM(a.shape, a.dtype) for a in held]
        + [
            pltpu.VMEM((n_tp, *out_weight.shape), bf16),
            pltpu.VMEM((rows, heads, width), f32),
            pltpu.VMEM((n_kv, owned, heads, width), f32),
            pltpu.VMEM((rows, 2, width), f32),
            pltpu.VMEM((n_kv, owned, 2, width), f32),
            pltpu.VMEM((rows, heads, width), bf16),
            pltpu.VMEM((rows, 2, width), bf16),
            pltpu.VMEM((rows, 2 * heads, width), bf16),
            pltpu.VMEM((rows, 2, width), f32),
            pltpu.VMEM((n_kv, owned, 2 * heads, width), bf16),
            pltpu.VMEM((n_kv, owned, 2, width), f32),
            pltpu.VMEM((n_tp, rows, heads, width), bf16),
            pltpu.VMEM((rows * heads, width), f32),
            pltpu.VMEM((rows, width, positions), bf16),
            pltpu.VMEM((rows, 1, positions), f32),
            dma((3 + len(held),)),
            dma((owners,)),
            dma((n_kv,)),
            dma((owners,)),
            dma((n_kv,)),
            dma((n_kv,)),
            dma((owners,)),
            dma((n_kv,)),
            dma((owners,)),
            dma((owners,)),
            dma((n_kv,)),
            dma((owners,)),
            dma((n_kv,)),
            dma((n_kv * n_tp,)),
            dma((owners * n_tp,)),
            dma((n_tp,)),
            dma((n_tp,)),
        ],
        compiler_params=pltpu.CompilerParams(collective_id=0, has_side_effects=True),
    )(lengths, lambdas, *held, out_weight)
    mixed, new_keys, new_values = pl.pallas_call(
        emit,
        name="emit",
        out_shape=[jax.ShapeDtypeStruct(shape, bf16) for shape in shapes],
        in_specs=[vmem] * 3,
        out_specs=[hbm] * 3,
        scratch_shapes=[dma((3,))],
    )(*[pltpu.with_memory_space_constraint(r, pltpu.VMEM) for r in results])
    return (
        mixed,
        new_keys.reshape(rows, kv_heads, width),
        new_values.reshape(rows, kv_heads, width),
    )


def solution(mesh):
    return jax.shard_map(
        functools.partial(body, mesh.shape["kv"], mesh.shape["tp"]),
        mesh=mesh,
        in_specs=(
            P("dp", "kv"),
            P("dp"),
            P("kv", "tp"),
            P("kv", "tp"),
            P("kv", "tp"),
            P(),
            P(),
            P("tp"),
            P(),
            P("tp", "kv"),
            P("dp", "kv", "tp", None),
            P("dp", "kv", "tp", None),
        ),
        out_specs=(P("dp", "kv"), P("dp", "tp", None), P("dp", "tp", None)),
        check_vma=False,
    )
```
